32 devices in a mesh: ep: 8 (over z, x), tp: 4 (over y, core).
Axes of the slice: x: 2, y: 2, z: 4, core: 2. Of those that a mesh axis runs over, the one named last changes fastest.
Arguments:
- receptance: bfloat16 [4096, 2048], P('ep', 'tp'), may hold values from -6 to 6
- key_rows: bfloat16 [4096, 2048], P('ep', 'tp'), may hold values from -6 to 6
- value_rows: bfloat16 [4096, 2048], P('ep', 'tp'), may hold values from -6 to 6
- decay_input: bfloat16 [4096, 2048], P('ep', 'tp'), may hold values from -2.796875 to 2.796875
- learn_input: bfloat16 [4096, 2048], P('ep', 'tp'), may hold values from -12 to 4
- decay_base: float32 [2048], P('tp'), may hold values from -20 to -2
- decay_shift: float32 [4096, 32], P('ep', 'tp'), may hold values from -1 to 20
- channel_gain: float32 [2048], P('tp'), may hold values from 0.1 to 1.9
- out_weight: bfloat16 [2048, 2048], P('tp'), may hold values from -0.125 to 0.125
- expert_input: bfloat16 [4096, 2048], P(('ep', 'tp')), may hold values from -6 to 6
- expert_gain: float32 [2048], replicated, may hold values from 0.1 to 1.9
- routes: int32 [4096, 2], P(('ep', 'tp')), may hold values from 0 to 7, all different within a row; in each aligned block of 128 rows (0 to 127, 128 to 255, ...) at most 64 rows name the same one
- route_weight: float32 [4096, 2], P(('ep', 'tp')), may hold values from 0.1 to 1
- gate_weight: bfloat16 [8, 2048, 1024], P('ep', None, 'tp'), may hold values from -0.125 to 0.125
- up_weight: bfloat16 [8, 2048, 1024], P('ep', None, 'tp'), may hold values from -0.125 to 0.125
- down_weight: bfloat16 [8, 1024, 2048], P('ep', 'tp'), may hold values from -0.1875 to 0.1875
Outputs:
- mixer_out: bfloat16 [4096, 2048], P(('ep', 'tp'))
- expert_out: bfloat16 [4096, 2048], P(('ep', 'tp'))
The draws below stay inside these ranges and needn't reach their ends.
Inputs may be any that keep to these rules, and one draw needn't show every extreme that they name: `routes`: within the rows of one device (aligned blocks of 128 rows) no expert is named by more than 64 rows, and in every draw some block names some expert exactly 64 times. Each row names 2 different experts.
All inputs are finite; a program needn't handle non-finite values.
Results may differ from the reference program's by a relative error of at most 0.024.
Values may be sent and summed in bfloat16 or wider, within the bound.
A program may use at most 128 MiB of HBM per device.

```python
import math
import jax
import jax.numpy as jnp
import numpy as np
from jax import lax

D = 2048
HEADS = 32
HEAD = 64
CHANNELS = 2048
FF = 1024
EXPERTS = 8
TOPK = 2
TOK_DEV = 128
MIX_ROWS = 512
MICRO_TOKENS = 4096
CAP = 64
N_TP = 4


def fast_heads(key):
    ranking = jax.random.permutation(jax.random.fold_in(key, 101), HEADS)
    quick_count = HEADS // 2
    return jnp.repeat(ranking < quick_count, HEAD)


def draw_decay_base(key, part):
    quick = fast_heads(key)
    spread = jax.random.uniform(jax.random.fold_in(key, 102), (CHANNELS,), jnp.float32)
    slow_rates = -jnp.log(jnp.float32(MICRO_TOKENS)) - 2.0 - spread
    quick_rates = -3.9 + 1.3 * spread
    return jnp.where(quick, quick_rates, slow_rates).astype(jnp.float32)


def draw_decay_shift(key, part):
    blocks = MICRO_TOKENS // MIX_ROWS
    reach = 0.5
    levels = jax.random.uniform(jax.random.fold_in(key, 103), (blocks, HEADS), jnp.float32, -reach, reach)
    each_row_amount = jnp.repeat(levels, MIX_ROWS, axis=0)
    surge_locations = jax.random.randint(jax.random.fold_in(key, 104), (3,), 0, MICRO_TOKENS)
    surge_groups = jnp.any(jnp.arange(MICRO_TOKENS, dtype=jnp.int32)[:, None] == surge_locations[None, :], axis=1)
    table_height = jnp.log(jnp.float32(MICRO_TOKENS)) + 3.0
    return (each_row_amount + jnp.where(surge_groups, table_height, 0.0)[:, None]).astype(jnp.float32)


def draw_learn_input(key, part):
    quick = fast_heads(key)
    slow_mean = -jnp.log(jnp.float32(MICRO_TOKENS) / HEAD) - 1.0
    centre = jnp.where(quick, 0.0, slow_mean)
    jitter = jnp.clip(jax.random.normal(jax.random.fold_in(key, 105), (MICRO_TOKENS, CHANNELS), jnp.float32), -3.0, 3.0)
    return (centre[None, :] + jitter).astype(jnp.bfloat16)


def block_scale(own_key, shape, cuts, smallest, top_value):
    factor_of = 1.0
    for dim, shards_of in cuts:
        draws = jax.random.uniform(jax.random.fold_in(jax.random.fold_in(own_key, 6), dim), (shards_of,), jnp.float32, smallest / len(cuts), top_value / len(cuts))
        factor_of = factor_of * jnp.repeat(jnp.exp(draws), shape[dim] // shards_of).reshape((-1,) + (1,) * (len(shape) - 1 - dim))
    return factor_of


def assign_block(own_key, own, number, rows, count, top, most, lean):
    sequence = jax.random.permutation(own_key, count)
    packed, ordinary = load_shares(count, rows * top, most, lean, True), load_shares(count, rows * top, most, lean, False)
    places = jnp.arange(count)

    def named(lengths, turn):
        used = int((lengths > 0).sum())
        fixed = max(1, used // 4)
        shifted = fixed + (places - fixed + turn * (used - fixed)) % max(1, count - fixed)
        return jnp.zeros((count,), jnp.int32).at[sequence[jnp.where(places < fixed, places, shifted)]].set(jnp.asarray(lengths, jnp.int32))

    lengths = jnp.where(number % 4 == 0, named(packed, number // 4), named(ordinary, number - number // 4 - 1))
    mixed = jax.random.permutation(jax.random.fold_in(own, 3), count)
    giver, sink = mixed[0:count // 2 * 2:2], mixed[1:count // 2 * 2:2]
    slack = jnp.minimum(lengths[giver] - 1, most - lengths[sink]) // 2
    slack = jnp.where((giver == sequence[0]) | (sink == sequence[0]) | (lengths[sink] == 0), 0, jnp.maximum(slack, 0))
    shifted = jax.random.randint(jax.random.fold_in(own, 4), (count // 2,), 0, 1 << 20) % (slack + 1)
    lengths = lengths.at[giver].add(-shifted).at[sink].add(shifted)
    items = jnp.searchsorted(jnp.cumsum(lengths), jnp.arange(rows * top), side="right").astype(jnp.int32)
    listing = items.reshape(top, rows).T
    listing = listing[jax.random.permutation(jax.random.fold_in(own, 1), rows)]
    turn = jax.random.randint(jax.random.fold_in(own, 2), (rows, 1), 0, top)
    return jnp.take_along_axis(listing, (jnp.arange(top)[None, :] + turn) % top, axis=1)


def load_shares(number_of, total, most, lean, full):
    loads = [(1 << 20) // math.isqrt(grade ** lean) + 1 for grade in range(1, number_of + 1)]
    largest = most if full else min(most, max(-(-total // number_of), total * loads[0] // sum(loads)))
    least = 1 if total - largest >= number_of - 1 else 0
    given, rest = [largest] + [least] * (number_of - 1), total - largest - least * (number_of - 1)
    while rest > 0:
        free = [i for i in range(1, number_of) if given[i] < largest] or [i for i in range(1, number_of) if given[i] < most]
        mass, left = sum([loads[i] for i in free]), rest
        for i in free:
            addition = min(most - given[i], max(1, left * loads[i] // mass), rest)
            given[i] = given[i] + addition
            rest = rest - addition
    return np.array(given)


def noise(own_key, dims, deviation, limit, pieces=(), held_as=jnp.bfloat16):
    entries = deviation * jax.random.normal(own_key, dims, jnp.float32)
    if pieces:
        entries = entries * block_scale(own_key, dims, pieces, -0.22, 0.18)
    return jnp.clip(entries, -limit, limit).astype(held_as)


def setup_inputs(seed: int = 0) -> dict:
    key_list = jax.random.split(jax.random.key(seed), 17)
    receptance = noise(key_list[0], (MICRO_TOKENS, CHANNELS), 1.0, 6.0, ((0, 8), (1, 4)))
    key_rows = noise(key_list[1], (MICRO_TOKENS, CHANNELS), 1.0, 6.0, ((0, 8), (1, 4)))
    value_rows = noise(key_list[2], (MICRO_TOKENS, CHANNELS), 1.0, 6.0, ((0, 8), (1, 4)))
    decay_input = noise(key_list[3], (MICRO_TOKENS, CHANNELS), 0.7, 2.796875, ((0, 8), (1, 4)))
    learn_input = draw_learn_input(jax.random.fold_in(key_list[16], 71), 0)
    decay_base = draw_decay_base(jax.random.fold_in(key_list[16], 71), 0)
    decay_shift = draw_decay_shift(jax.random.fold_in(key_list[16], 71), 0)
    channel_gain = jnp.clip(1.0 + 0.18 * jax.random.normal(key_list[7], (CHANNELS,), jnp.float32), 0.1, 1.9)
    out_weight = noise(key_list[8], (CHANNELS, D), CHANNELS ** -0.5, 0.125, ((0, 4),))
    expert_input = noise(key_list[9], (MICRO_TOKENS, D), 1.0, 6.0, ((0, 32),))
    expert_gain = jnp.clip(1.0 + 0.18 * jax.random.normal(key_list[10], (D,), jnp.float32), 0.1, 1.9)
    routes_keys = jax.random.split(jax.random.fold_in(key_list[11], 1), MICRO_TOKENS // TOK_DEV)
    routes_turns = jax.random.permutation(jax.random.fold_in(key_list[11], 3), MICRO_TOKENS // TOK_DEV)
    routes = jax.vmap(lambda own, number: assign_block(jax.random.fold_in(key_list[11], 2), own, number, TOK_DEV, EXPERTS, TOPK, CAP, 1))(routes_keys, routes_turns).reshape((MICRO_TOKENS, TOPK))
    route_weight = jnp.clip(jnp.exp(math.log(1.0) - 2.3025851 * jax.random.uniform(key_list[12], (MICRO_TOKENS, TOPK), jnp.float32) ** block_scale(key_list[12], (MICRO_TOKENS, TOPK), ((0, 32),), -0.2, 0.2)), 0.1, 1.0)
    gate_weight = noise(key_list[13], (EXPERTS, D, FF), D ** -0.5, 0.125, ((0, 8), (2, 4)))
    up_weight = noise(key_list[14], (EXPERTS, D, FF), D ** -0.5, 0.125, ((0, 8), (2, 4)))
    down_weight = noise(key_list[15], (EXPERTS, FF, D), FF ** -0.5, 0.1875, ((0, 8), (1, 4)))
    return {"receptance": receptance, "key_rows": key_rows, "value_rows": value_rows, "decay_input": decay_input, "learn_input": learn_input, "decay_base": decay_base, "decay_shift": decay_shift, "channel_gain": channel_gain, "out_weight": out_weight, "expert_input": expert_input, "expert_gain": expert_gain, "routes": routes, "route_weight": route_weight, "gate_weight": gate_weight, "up_weight": up_weight, "down_weight": down_weight}


NORM_EPS = 1e-06
GROUP_EPS = 0.00064
KEY_EPS = 1e-06
PRECISE = lax.Precision.HIGHEST

def rounded_sum(inputs, weight, groups):
    group_size = inputs.shape[1] // groups
    result = jnp.zeros((inputs.shape[0], weight.shape[1]), jnp.float32)
    for part_index in range(groups):
        lower = part_index * group_size
        partial_value = jnp.dot(inputs[:, lower:lower + group_size], weight[lower:lower + group_size], preferred_element_type=jnp.float32)
        result = result + lax.optimization_barrier(partial_value.astype(jnp.bfloat16)).astype(jnp.float32)
    return result.astype(jnp.bfloat16)

def slot_targets(block_routes, experts, capacity):
    flat_routes = block_routes.reshape(-1)
    matches = (flat_routes[:, None] == jnp.arange(experts, dtype=jnp.int32)[None, :]).astype(jnp.int32)
    earlier = jnp.cumsum(matches, axis=0) - matches
    slots = lax.optimization_barrier(jnp.sum(earlier * matches, axis=1)).reshape(block_routes.shape)
    return (block_routes * capacity + slots).astype(jnp.int32)

def token_mixer(receptance, key_rows, value_rows, decay_input, learn_input, decay_base, decay_shift, channel_gain, out_weight):
    head_shape = (MICRO_TOKENS, HEADS, HEAD)
    recept = receptance.astype(jnp.float32).reshape(head_shape)
    key_data = key_rows.astype(jnp.float32).reshape(head_shape)
    value_data = value_rows.astype(jnp.float32).reshape(head_shape)
    pre_decay = decay_input.astype(jnp.float32).reshape(head_shape) + decay_base.reshape(1, HEADS, HEAD) + decay_shift[:, :, None]
    decays = jnp.exp(-jnp.exp(-jax.nn.softplus(-pre_decay) - 0.5))
    rates = jax.nn.sigmoid(learn_input.astype(jnp.float32)).reshape(head_shape)
    unit_keys = key_data / jnp.sqrt(lax.optimization_barrier(jnp.sum(key_data * key_data, axis=2, keepdims=True)) + KEY_EPS)
    removal = unit_keys * rates

    def advance(state, inputs):
        recept_now, decay_now, key_now, value_now, unit_now, removal_now = inputs
        probes = jnp.einsum('hij,hj->hi', state, unit_now, precision=PRECISE)
        state = state * decay_now[:, None, :] - probes[:, :, None] * removal_now[:, None, :] + value_now[:, :, None] * key_now[:, None, :]
        return (state, jnp.einsum('hij,hj->hi', state, recept_now, precision=PRECISE))
    start_state = jnp.zeros((HEADS, HEAD, HEAD), jnp.float32)
    _, readout = lax.scan(advance, start_state, (recept, decays, key_data, value_data, unit_keys, removal))
    centred = readout - lax.optimization_barrier(jnp.mean(readout, axis=2, keepdims=True))
    variance = lax.optimization_barrier(jnp.mean(centred * centred, axis=2, keepdims=True))
    normed = (centred * lax.rsqrt(variance + GROUP_EPS)).reshape(MICRO_TOKENS, CHANNELS) * channel_gain
    return rounded_sum(normed.astype(jnp.bfloat16), out_weight, N_TP)

def expert_layer(expert_input, expert_gain, routes, route_weight, gate_weight, up_weight, down_weight):
    inputs = expert_input.astype(jnp.float32)
    normed = (inputs * lax.rsqrt(lax.optimization_barrier(jnp.mean(inputs * inputs, axis=1, keepdims=True)) + NORM_EPS) * expert_gain).astype(jnp.bfloat16)
    blocks = MICRO_TOKENS // TOK_DEV
    block_routes = routes.reshape(blocks, TOK_DEV, TOPK)
    targets = jax.vmap(lambda member: slot_targets(member, EXPERTS, CAP))(block_routes)
    slots = targets - block_routes * CAP
    block_index = jnp.arange(blocks, dtype=jnp.int32)[:, None, None]
    places = ((block_routes * blocks + block_index) * CAP + slots).astype(jnp.int32)
    token_index = jnp.broadcast_to(jnp.arange(MICRO_TOKENS, dtype=jnp.int32).reshape(blocks, TOK_DEV, 1), places.shape)
    owners = jnp.full((EXPERTS * blocks * CAP,), MICRO_TOKENS, jnp.int32).at[places.reshape(-1)].set(token_index.reshape(-1))
    padded = jnp.concatenate([normed, jnp.zeros((1, D), jnp.bfloat16)], axis=0)

    def run_expert(operands):
        owner_rows, w_gate, w_up, w_down = operands
        gathered = padded[owner_rows]
        gates = jnp.dot(gathered, w_gate, preferred_element_type=jnp.float32)
        uppers = jnp.dot(gathered, w_up, preferred_element_type=jnp.float32)
        hidden = (jax.nn.silu(gates) * uppers).astype(jnp.bfloat16)
        return rounded_sum(hidden, w_down, N_TP)
    outputs = lax.map(run_expert, (owners.reshape(EXPERTS, blocks * CAP), gate_weight, up_weight, down_weight))
    flat_rows = outputs.reshape(EXPERTS * blocks * CAP, D)
    picks = places.reshape(MICRO_TOKENS, TOPK)
    combined = jnp.zeros((MICRO_TOKENS, D), jnp.float32)
    for picked in range(TOPK):
        combined = combined + flat_rows[picks[:, picked]].astype(jnp.float32) * route_weight[:, picked:picked + 1]
    return combined.astype(jnp.bfloat16)

def reference(receptance, key_rows, value_rows, decay_input, learn_input, decay_base, decay_shift, channel_gain, out_weight, expert_input, expert_gain, routes, route_weight, gate_weight, up_weight, down_weight):
    mixer_out = token_mixer(receptance, key_rows, value_rows, decay_input, learn_input, decay_base, decay_shift, channel_gain, out_weight)
    expert_out = expert_layer(expert_input, expert_gain, routes, route_weight, gate_weight, up_weight, down_weight)
    return (mixer_out, expert_out)
```

```python
import functools

import jax
import jax.numpy as jnp
from jax import lax
from jax.experimental import pallas as pl
from jax.experimental.pallas import tpu as pltpu
from jax.sharding import PartitionSpec as P

SPAN = 128
STACK = 2
LANES = 128

NORM_EPS = 1e-06
GROUP_EPS = 0.00064
KEY_EPS = 1e-06
F32 = jnp.float32
BF16 = jnp.bfloat16


def mm(a, b):
    return lax.dot_general(
        a.astype(BF16), b.astype(BF16), (((1,), (0,)), ((), ())), preferred_element_type=F32
    )


def mm_nt(a, b):
    return lax.dot_general(
        a.astype(BF16), b.astype(BF16), (((1,), (1,)), ((), ())), preferred_element_type=F32
    )


def mm_tn(a, b):
    return lax.dot_general(
        a.astype(BF16), b.astype(BF16), (((0,), (0,)), ((), ())), preferred_element_type=F32
    )


def split_two(x):
    high = x.astype(BF16)
    return high, (x - high.astype(F32)).astype(BF16)


def grid_index(shape, axis):
    return lax.broadcasted_iota(jnp.int32, shape, axis)


def same_head(head_size):
    rows = grid_index((LANES, LANES), 0) // head_size
    cols = grid_index((LANES, LANES), 1) // head_size
    return rows == cols


def head_sums(x, block):
    high, low = split_two(x)
    return mm(
        jnp.concatenate([high, low], axis=1), jnp.concatenate([block, block], axis=0)
    )


def lower_inverses(strict_parts, rows, cols):
    eye = jnp.where(rows == cols, 1.0, 0.0)
    size = 1
    inverses = None
    while size < SPAN:
        off = (rows // (2 * size) == cols // (2 * size)) & (rows // size != cols // size)
        parts = [jnp.where(off, part, 0.0) for part in strict_parts]
        if inverses is None:
            inverses = [eye - part for part in parts]
        else:
            firsts = [mm(part, inv) for part, inv in zip(parts, inverses)]
            inverses = [inv - mm(inv, first) for inv, first in zip(inverses, firsts)]
        size *= 2
    return inverses


def local_kernel(
    head_size,
    r_ref,
    k_ref,
    v_ref,
    d_ref,
    l_ref,
    base_ref,
    shift_ref,
    reader_ref,
    local_ref,
    summary_ref,
    state,
):
    pair = pl.program_id(0)
    half = LANES // 2

    rows = grid_index((SPAN, SPAN), 0)
    cols = grid_index((SPAN, SPAN), 1)
    strict = rows > cols
    inclusive = rows >= cols
    first = grid_index((SPAN, LANES), 1) < half
    matched = same_head(head_size)
    block = matched.astype(BF16)
    diagonal = grid_index((LANES, LANES), 0) == grid_index((LANES, LANES), 1)
    tri = inclusive.astype(BF16)
    tri_two = jnp.concatenate([tri, tri], axis=1)

    state[:LANES] = jnp.zeros((LANES, LANES), F32)
    state[LANES:] = jnp.where(diagonal, 1.0, 0.0)

    heads = shift_ref.shape[1]
    chosen = grid_index((heads, LANES), 0) == 2 * pair + grid_index((heads, LANES), 1) // half
    def advance(step, nothing):
        start = pl.multiple_of(step * (STACK * SPAN), STACK * SPAN)
        rows_here = pl.ds(start, STACK * SPAN)
        shift = lax.dot_general(
            shift_ref[rows_here],
            chosen.astype(F32),
            (((1,), (0,)), ((), ())),
            precision=lax.Precision.HIGHEST,
            preferred_element_type=F32,
        )
        pre = d_ref[rows_here].astype(F32) + base_ref[0] + shift
        log_all = -0.6065306597126334 / (1.0 + jnp.exp(-pre))
        rates = 1.0 / (1.0 + jnp.exp(-l_ref[rows_here].astype(F32)))
        key_all = k_ref[rows_here].astype(F32)
        unit_all = key_all * lax.rsqrt(head_sums(key_all * key_all, block) + KEY_EPS)
        removal_all = unit_all * rates

        spans = STACK
        items = []
        strict_parts = []
        for j in range(spans):
            here = slice(j * SPAN, (j + 1) * SPAN)
            log_decay = log_all[here]
            high, low = split_two(log_decay)
            cum = mm(tri_two, jnp.concatenate([high, low], axis=0))
            middle = cum[SPAN // 2 - 1 : SPAN // 2]
            ending = cum[SPAN - 1 :]
            e_cm = jnp.exp(cum - middle)
            e_pm = jnp.exp(cum - log_decay - middle)
            shrink = jnp.exp(middle - cum)
            e_mid = jnp.exp(middle)
            e_tail = jnp.exp(ending - middle)
            unit, key = unit_all[here], key_all[here]
            value = v_ref[pl.ds(start + j * SPAN, SPAN)]
            turned = jnp.concatenate([value[:, half:], value[:, :half]], axis=1)
            recept = r_ref[pl.ds(start + j * SPAN, SPAN)].astype(F32)
            probes = unit * e_pm
            queries = recept * e_cm
            back_removal = removal_all[here] * shrink
            back_keys = key * shrink
            left = jnp.concatenate(
                [
                    jnp.where(first, probes, 0.0),
                    jnp.where(first, 0.0, probes),
                    jnp.where(first, queries, 0.0),
                    jnp.where(first, 0.0, queries),
                ],
                axis=0,
            )
            products = mm_nt(left, jnp.concatenate([back_removal, back_keys], axis=0))
            for h in range(2):
                strict_parts.append(
                    jnp.where(strict, products[h * SPAN : (h + 1) * SPAN, :SPAN], 0.0)
                )
            items.append(
                dict(
                    products=products,
                    turned=turned,
                    carrying=probes * e_mid,
                    reading=queries * e_mid,
                    removal_tail=back_removal * e_tail,
                    key_tail=back_keys * e_tail,
                    fade=jnp.exp(ending),
                )
            )
        inverses = lower_inverses(strict_parts, rows, cols)
        for j in range(spans):
            item = items[j]
            products, turned = item["products"], item["turned"]
            solved, removed, kept = [], [], []
            for h in range(2):
                top = slice(h * SPAN, (h + 1) * SPAN)
                bottom = slice((2 + h) * SPAN, (3 + h) * SPAN)
                pair_keys = jnp.where(strict, products[top, SPAN:], 0.0)
                read_removal = jnp.where(inclusive, products[bottom, :SPAN], 0.0)
                read_keys = jnp.where(inclusive, products[bottom, SPAN:], 0.0)
                both = mm(jnp.concatenate([pair_keys, read_keys], axis=0), turned)
                own = first if h == 0 else jnp.logical_not(first)
                right = jnp.where(own, item["carrying"], both[:SPAN])
                answer = mm(inverses[2 * j + h], right)
                solved.append(answer)
                removed.append(mm(read_removal, answer))
                kept.append(both[SPAN:])
            carried = jnp.where(first, solved[0], solved[1])
            local_turned = jnp.where(first, solved[1], solved[0])
            reader = item["reading"] - jnp.where(first, removed[0], removed[1])
            read_turned = jnp.where(first, kept[1] - removed[1], kept[0] - removed[0])
            local_read = jnp.concatenate([read_turned[:, half:], read_turned[:, :half]], axis=1)
            taken = mm_tn(
                jnp.concatenate([carried, local_turned], axis=1), item["removal_tail"]
            )
            offset_turned = mm_tn(turned, item["key_tail"]) - taken[LANES:]
            offset = jnp.concatenate([offset_turned[half:], offset_turned[:half]], axis=0)
            offset = jnp.where(matched, offset, 0.0)
            transition = jnp.where(diagonal, item["fade"], 0.0) - jnp.where(
                matched, taken[:LANES], 0.0
            )
            now = state[...]
            reads = mm_nt(reader, now)
            here = pl.ds(start + j * SPAN, SPAN)
            local_ref[here] = local_read + reads[:, :LANES]
            reader_ref[pl.ds(start + j * SPAN, SPAN)] = reads[:, LANES:].astype(BF16)
            now_high, now_low = split_two(now)
            step_high, step_low = split_two(transition)
            moved = mm(now_high, step_high) + mm(now_low, step_high) + mm(now_high, step_low)
            state[:LANES] = moved[:LANES] + offset
            state[LANES:] = moved[LANES:]
        return nothing

    lax.fori_loop(0, r_ref.shape[0] // (STACK * SPAN), advance, 0)
    summary_ref[1] = (state[:half] + state[half:LANES]).astype(BF16)
    summary_ref[0] = (state[LANES : LANES + half] + state[LANES + half :]).astype(BF16)


def mixer_local(receptance, keys, values, decay, learn, base, shift, head_size):
    rows, channels = receptance.shape
    pairs = channels // LANES
    heads = shift.shape[1]
    half = LANES // 2
    tile = pl.BlockSpec((rows, LANES), lambda p: (0, p))
    small = pl.BlockSpec((2, half, LANES), lambda p: (0, p, 0))
    return pl.pallas_call(
        functools.partial(local_kernel, head_size),
        grid=(pairs,),
        in_specs=[tile] * 5
        + [
            pl.BlockSpec((1, 1, LANES), lambda p: (p, 0, 0)),
            pl.BlockSpec((rows, heads), lambda p: (0, 0)),
        ],
        out_specs=[tile, tile, small],
        out_shape=[
            jax.ShapeDtypeStruct((rows, channels), BF16),
            jax.ShapeDtypeStruct((rows, channels), F32),
            jax.ShapeDtypeStruct((2, pairs * half, LANES), BF16),
        ],
        scratch_shapes=[pltpu.VMEM((2 * LANES, LANES), F32)],
        compiler_params=pltpu.CompilerParams(
            dimension_semantics=("arbitrary",), vmem_limit_bytes=24 * 2**20
        ),
        cost_estimate=pl.CostEstimate(
            flops=20 * 10**9, bytes_accessed=6 * 2**20, transcendentals=10**6
        ),
        name="mixer_local",
    )(receptance, keys, values, decay, learn, base.reshape(pairs, 1, LANES), shift)


def finish_kernel(
    head_size,
    summary_ref,
    reader_ref,
    local_ref,
    gain_ref,
    out_ref,
    landed,
    send_sems,
    recv_sems,
):
    here = lax.axis_index("ep")
    count = lax.axis_size("ep")
    half = LANES // 2
    rows, channels = reader_ref.shape
    pairs = channels // LANES
    matched = same_head(head_size)
    block = matched.astype(BF16)

    def transfer(distance, target):
        return pltpu.make_async_remote_copy(
            src_ref=summary_ref,
            dst_ref=landed.at[distance - 1],
            send_sem=send_sems.at[distance - 1],
            recv_sem=recv_sems.at[distance - 1],
            device_id={"ep": target},
            device_id_type=pl.DeviceIdType.MESH,
        )

    barrier = pltpu.get_barrier_semaphore()

    def greet(distance, nothing):
        pl.semaphore_signal(
            barrier,
            inc=1,
            device_id={"ep": lax.rem(here + distance, count)},
            device_id_type=pl.DeviceIdType.MESH,
        )
        return nothing

    lax.fori_loop(1, count, greet, 0)
    pl.semaphore_wait(barrier, count - 1)

    def launch(distance, nothing):
        transfer(distance, here + distance).start()
        return nothing

    lax.fori_loop(1, count - here, launch, 0)

    def wide(place, kind, p):
        part = landed[place, kind, p * half : (p + 1) * half].astype(F32)
        return jnp.where(matched, jnp.concatenate([part, part], axis=0), 0.0)

    def turn(k, states):
        distance = here - k
        transfer(distance, k).wait_recv()
        after = []
        for p in range(pairs):
            high, low = split_two(states[p])
            moved = mm(jnp.concatenate([high, low], axis=0), wide(distance - 1, 0, p))
            after.append(moved[:LANES] + moved[LANES:] + wide(distance - 1, 1, p))
        return tuple(after)

    nothing = tuple(jnp.zeros((LANES, LANES), F32) for _ in range(pairs))
    entering = lax.fori_loop(0, here, turn, nothing)
    for p in range(pairs):
        lanes = slice(p * LANES, (p + 1) * LANES)
        read = mm_nt(reader_ref[:, lanes], entering[p]) + local_ref[:, lanes]
        centred = read - head_sums(read, block) * (1.0 / head_size)
        variance = head_sums(centred * centred, block) * (1.0 / head_size)
        scaled = centred * lax.rsqrt(variance + GROUP_EPS) * gain_ref[:, lanes]
        out_ref[:, lanes] = scaled.astype(BF16)

    def settle(distance, nothing):
        transfer(distance, here + distance).wait_send()
        return nothing

    lax.fori_loop(1, count - here, settle, 0)


def mixer_finish(summary, reader, local_read, gain, head_size):
    rows, channels = reader.shape
    count = lax.axis_size("ep")
    return pl.pallas_call(
        functools.partial(finish_kernel, head_size),
        in_specs=[pl.BlockSpec(memory_space=pltpu.VMEM)] * 4,
        out_specs=pl.BlockSpec(memory_space=pltpu.VMEM),
        out_shape=jax.ShapeDtypeStruct((rows, channels), BF16),
        scratch_shapes=[
            pltpu.VMEM((count - 1,) + summary.shape, BF16),
            pltpu.SemaphoreType.DMA((count - 1,)),
            pltpu.SemaphoreType.DMA((count - 1,)),
        ],
        compiler_params=pltpu.CompilerParams(
            vmem_limit_bytes=32 * 2**20, collective_id=0, has_side_effects=True
        ),
        cost_estimate=pl.CostEstimate(
            flops=10 * 10**9, bytes_accessed=4 * 2**20, transcendentals=10**5
        ),
        name="mixer_finish",
    )(summary, reader, local_read, gain.reshape(1, channels))


def hidden_kernel(x_ref, gate_ref, up_ref, out_ref):
    gates = mm(x_ref[...], gate_ref[0])
    uppers = mm(x_ref[...], up_ref[0])
    out_ref[...] = (gates / (1.0 + jnp.exp(-gates)) * uppers).astype(BF16)


def expert_hidden(incoming, all_gate, all_up):
    rows, width = incoming.shape
    shards, _, units = all_gate.shape
    weight = pl.BlockSpec((1, width, units), lambda t: (t, 0, 0))
    return pl.pallas_call(
        hidden_kernel,
        grid=(shards,),
        in_specs=[pl.BlockSpec((rows, width), lambda t: (0, 0)), weight, weight],
        out_specs=pl.BlockSpec((rows, units), lambda t: (0, t)),
        out_shape=jax.ShapeDtypeStruct((rows, shards * units), BF16),
        compiler_params=pltpu.CompilerParams(
            dimension_semantics=("arbitrary",), vmem_limit_bytes=32 * 2**20
        ),
        cost_estimate=pl.CostEstimate(
            flops=4 * rows * width * units * shards,
            bytes_accessed=2 * (rows * width + 2 * shards * units * width),
            transcendentals=rows * units * shards,
        ),
        name="expert_hidden",
    )(incoming, all_gate, all_up)


def slot_targets(block_routes, experts, capacity):
    flat_routes = block_routes.reshape(-1)
    count = flat_routes.shape[0]
    order = jnp.arange(count, dtype=jnp.int32)
    before = (order[:, None] > order[None, :]) & (flat_routes[:, None] == flat_routes[None, :])
    slots = jnp.sum(before.astype(jnp.int32), axis=1).reshape(block_routes.shape)
    return block_routes * capacity + slots


def dispersal_table(targets, places):
    marks = (jnp.arange(places, dtype=jnp.int32)[:, None, None] == targets[None, :, :]).astype(
        jnp.int32
    )
    return jnp.sum(marks, axis=2).astype(jnp.bfloat16)


def on_device(
    receptance,
    key_rows,
    value_rows,
    decay_input,
    learn_input,
    decay_base,
    decay_shift,
    channel_gain,
    out_weight,
    expert_input,
    expert_gain,
    routes,
    route_weight,
    gate_weight,
    up_weight,
    down_weight,
):
    ep_count = lax.axis_size("ep")
    channels = receptance.shape[1]
    head_size = channels // decay_shift.shape[1]
    token_rows, model_width = expert_input.shape
    top_count = routes.shape[1]
    experts = gate_weight.shape[0] * ep_count
    capacity = max(2, 2 * token_rows * top_count // experts)
    slab_rows = ep_count * capacity

    all_gate = lax.all_gather(gate_weight[0], "tp")
    all_up = lax.all_gather(up_weight[0], "tp")
    all_down = lax.all_gather(down_weight[0], "tp")

    inputs = expert_input.astype(F32)
    expert_normed = (
        inputs
        * lax.rsqrt(jnp.mean(inputs * inputs, axis=1, keepdims=True) + NORM_EPS)
        * expert_gain
    ).astype(BF16)
    own_targets = slot_targets(routes, experts, capacity)
    outgoing = jnp.dot(
        dispersal_table(own_targets, experts * capacity),
        expert_normed,
        preferred_element_type=F32,
    ).astype(BF16)
    arrived = lax.all_to_all(
        outgoing.reshape(experts, capacity, model_width),
        "ep",
        split_axis=0,
        concat_axis=0,
        tiled=True,
    ).reshape(slab_rows, model_width)

    reader, local_read, summary = mixer_local(
        receptance,
        key_rows,
        value_rows,
        decay_input,
        learn_input,
        decay_base,
        decay_shift,
        head_size,
    )
    mixed = mixer_finish(summary, reader, local_read, channel_gain, head_size)
    mixer_term = jnp.dot(mixed, out_weight, preferred_element_type=F32)
    mixer_out = lax.psum_scatter(
        mixer_term.astype(BF16), "tp", scatter_dimension=0, tiled=True
    )

    hidden = expert_hidden(arrived, all_gate, all_up)
    total = jnp.dot(
        hidden, all_down.reshape(hidden.shape[1], model_width), preferred_element_type=F32
    )
    returned = lax.all_to_all(
        total.astype(BF16).reshape(ep_count, capacity, model_width),
        "ep",
        split_axis=0,
        concat_axis=0,
        tiled=True,
    )
    flat_rows = returned.reshape(experts * capacity, model_width)
    places = jnp.arange(experts * capacity, dtype=jnp.int32)
    combined = jnp.zeros((token_rows, model_width), F32)
    for picked in range(top_count):
        table = (own_targets[:, picked : picked + 1] == places[None, :]).astype(BF16)
        chosen = jnp.dot(table, flat_rows, preferred_element_type=F32)
        combined = combined + chosen * route_weight[:, picked : picked + 1]
    return (mixer_out, combined.astype(BF16))


def solution(mesh):
    return jax.shard_map(
        on_device,
        mesh=mesh,
        in_specs=(
            P("ep", "tp"),
            P("ep", "tp"),
            P("ep", "tp"),
            P("ep", "tp"),
            P("ep", "tp"),
            P("tp"),
            P("ep", "tp"),
            P("tp"),
            P("tp", None),
            P(("ep", "tp"), None),
            P(),
            P(("ep", "tp"), None),
            P(("ep", "tp"), None),
            P("ep", None, "tp"),
            P("ep", None, "tp"),
            P("ep", "tp", None),
        ),
        out_specs=(P(("ep", "tp"), None), P(("ep", "tp"), None)),
        check_vma=False,
    )
```
